32 devices in a mesh: grp: 2 (over y), fs: 4 (over z), tp: 4 (over x, core).
Axes of the slice: x: 2, y: 2, z: 4, core: 2. Of those that a mesh axis runs over, the one named last changes fastest.
Arguments:
- incoming_representations: bfloat16 [5120, 2048], P(('grp', 'fs', 'tp')), parts along dimension 0, may hold values from -6 to 6
- perceptron_switch_coefficients: bfloat16 [2048, 5120], P('fs', 'tp'), may hold values from -0.125 to 0.125
- perceptron_expand_coefficients: bfloat16 [2048, 5120], P('fs', 'tp'), may hold values from -0.125 to 0.125
- perceptron_contract_coefficients: bfloat16 [5120, 2048], P('tp', 'fs'), may hold values from -0.5 to 0.5
- probe_coefficients: bfloat16 [2048, 512], P('fs', 'tp'), may hold values from -0.125 to 0.125
- address_coefficients: bfloat16 [2048, 512], P('fs', 'tp'), may hold values from -0.125 to 0.125
- payload_coefficients: bfloat16 [2048, 1024], P('fs', 'tp'), may hold values from -0.125 to 0.125
- emit_switch_coefficients: bfloat16 [2048, 1024], P('fs', 'tp'), may hold values from -0.125 to 0.125
- forgetting_shrink_coefficients: bfloat16 [2048, 32], replicated, may hold values from -0.125 to 0.125
- forgetting_expand_coefficients: bfloat16 [32, 512], P(None, 'tp'), may hold values from -3 to 3
- forgetting_sigmoid_intercept: float32 [512], P('tp'), may hold values from -1 to 9
- extra_forgetting_logits: float32 [5120, 512], P(('grp', 'fs'), 'tp'), parts along dimension 0, may hold values from -0.7 to 0
- subspace_rescaling_amplitude: float32 [128], replicated, may hold values from 0.1 to 1.9
- recurrence_emit_coefficients: bfloat16 [1024, 2048], P('tp', 'fs'), may hold values from -0.5 to 0.5
Outputs:
- layer_out: bfloat16 [5120, 2048], P(('grp', 'fs', 'tp')), parts along dimension 0
The draws below stay inside these ranges and needn't reach their ends.
There are 2 independent parts, one for each index of `grp`. The reference program is written for one: setup_inputs(seed, part) draws one part's arguments, and reference() takes and returns one part's arrays. A program takes and returns all parts, laid end to end along the dimension named above; an argument that names none is the same for every part. Nothing has to cross between parts.
All inputs are finite; a program needn't handle non-finite values.
Results may differ from the reference program's by a relative error of at most 0.035.
Values may be sent and summed in bfloat16 or wider, within the bound.
No kernel may reach another device: no remote copies, remote signals or barrier semaphores. Data moves between devices by JAX's collectives and lax.ppermute only.
A program may use at most 64 MiB of HBM per device.

```python
import math
import jax
import jax.numpy as jnp
from jax import lax

D = 2048
FF = 5120
HEADS = 8
DK = 64
DV = 128
RANK = 32
BLOCK = 64
SEQUENCE_LENGTH = 320
TOKEN_TOTAL = 2560
N_TP = 4


def draw_forgetting_sigmoid_intercept(key, part):
    channels = HEADS * DK
    sequence_streams = jax.random.split(jax.random.fold_in(key, 7), 3)
    percent = 50
    chosen = (jax.random.randint(sequence_streams[0], (channels,), 0, 100) < percent).astype(jnp.float32)
    fast_bias = jax.random.uniform(sequence_streams[1], (channels,), jnp.float32, -1.0, 0.8)
    slow_bias = jax.random.uniform(sequence_streams[2], (channels,), jnp.float32, 5.0, 9.0)
    return chosen * fast_bias + (1.0 - chosen) * slow_bias


def draw_extra_forgetting_logits(key, part):
    channels = HEADS * DK
    sequence_streams = jax.random.split(jax.random.fold_in(key, 11), 4)
    sequence_total = TOKEN_TOTAL // SEQUENCE_LENGTH
    spike_first = jax.random.randint(sequence_streams[0], (sequence_total, 1), 0, SEQUENCE_LENGTH)
    spike_second = jax.random.randint(sequence_streams[1], (sequence_total, 1), 0, SEQUENCE_LENGTH)
    token_positions = jnp.arange(SEQUENCE_LENGTH)[None, :]
    spike_mask = ((token_positions == spike_first) | (token_positions == spike_second)).astype(jnp.float32).reshape(TOKEN_TOTAL, 1)
    spike_strength = jax.random.uniform(sequence_streams[2], (TOKEN_TOTAL, channels), jnp.float32, 0.22, 0.69)
    block_total = TOKEN_TOTAL // BLOCK
    decay_offset_term = jnp.exp(jax.random.uniform(sequence_streams[3], (block_total, 1, channels), jnp.float32, math.log(0.0002), math.log(0.003)))
    decay_offset_term = jnp.broadcast_to(decay_offset_term, (block_total, BLOCK, channels)).reshape(TOKEN_TOTAL, channels)
    return -(spike_mask * spike_strength + decay_offset_term)


def block_scale(own_key, shape, pieces, low, largest):
    gain = 1.0
    for position, parts in pieces:
        heights = jax.random.uniform(jax.random.fold_in(jax.random.fold_in(own_key, 6), position), (parts,), jnp.float32, low / len(pieces), largest / len(pieces))
        gain = gain * jnp.repeat(jnp.exp(heights), shape[position] // parts).reshape((-1,) + (1,) * (len(shape) - 1 - position))
    return gain


def bell_draw(stream_key, shape, width, limit, pieces=(), kind=jnp.bfloat16):
    loudness = block_scale(stream_key, shape, pieces, -0.22, 0.18) if pieces else 1.0
    values = jax.random.normal(stream_key, shape, jnp.float32) * width * loudness
    return jnp.minimum(jnp.maximum(values, -limit), limit).astype(kind)


def setup_inputs(seed: int = 0, part: int = 0) -> dict:
    seeds = jax.random.split(jax.random.key(seed), 15)
    part_splits = jax.random.split(jax.random.fold_in(seeds[14], part), 15)
    return {
        "incoming_representations": bell_draw(part_splits[0], (TOKEN_TOTAL, D), 1.0, 6.0, ((0, 16),)),
        "perceptron_switch_coefficients": bell_draw(seeds[1], (D, FF), D ** -0.5, 0.125, ((0, 4), (1, 4))),
        "perceptron_expand_coefficients": bell_draw(seeds[2], (D, FF), D ** -0.5, 0.125, ((0, 4), (1, 4))),
        "perceptron_contract_coefficients": bell_draw(seeds[3], (FF, D), (max(FF // 36, 1)) ** -0.5, 0.5, ((0, 4), (1, 4))),
        "probe_coefficients": bell_draw(seeds[4], (D, HEADS * DK), D ** -0.5, 0.125, ((0, 4), (1, 4))),
        "address_coefficients": bell_draw(seeds[5], (D, HEADS * DK), D ** -0.5, 0.125, ((0, 4), (1, 4))),
        "payload_coefficients": bell_draw(seeds[6], (D, HEADS * DV), D ** -0.5, 0.125, ((0, 4), (1, 4))),
        "emit_switch_coefficients": bell_draw(seeds[7], (D, HEADS * DV), D ** -0.5, 0.125, ((0, 4), (1, 4))),
        "forgetting_shrink_coefficients": bell_draw(seeds[8], (D, RANK), D ** -0.5, 0.125),
        "forgetting_expand_coefficients": bell_draw(seeds[9], (RANK, HEADS * DK), (3 * RANK ** -0.5), 3.0, ((1, 4),)),
        "forgetting_sigmoid_intercept": draw_forgetting_sigmoid_intercept(jax.random.fold_in(seeds[14], 71), part),
        "extra_forgetting_logits": draw_extra_forgetting_logits(jax.random.fold_in(jax.random.fold_in(seeds[14], part), 71), part),
        "subspace_rescaling_amplitude": jnp.clip(1.0 + 0.18 * jax.random.normal(seeds[12], (DV,), jnp.float32), 0.1, 1.9),
        "recurrence_emit_coefficients": bell_draw(seeds[13], (HEADS * DV, D), (max(HEADS * DV // 9, 1)) ** -0.5, 0.5, ((0, 4), (1, 4))),
    }


residual_gain = 1.681792830507429
forgetting_steepness_multiplier = 16.0
epsilon = 1e-06
highest = lax.Precision.HIGHEST

def post_norm(residual, branch):
    summed = residual_gain * residual.astype(jnp.float32) + branch
    average = lax.optimization_barrier(jnp.mean(summed, axis=-1, keepdims=True))
    centred = summed - average
    variance = lax.optimization_barrier(jnp.mean(centred * centred, axis=-1, keepdims=True))
    return (centred * lax.rsqrt(variance + epsilon)).astype(jnp.bfloat16)

def rounded_sum(hidden, weight):
    block_width = hidden.shape[1] // N_TP
    totals = jnp.zeros((hidden.shape[0], weight.shape[1]), jnp.float32)
    for block_index in range(N_TP):
        begin = block_index * block_width
        partial_value = jnp.dot(hidden[:, begin:begin + block_width], weight[begin:begin + block_width], preferred_element_type=jnp.float32)
        partial_value = lax.optimization_barrier(partial_value.astype(jnp.bfloat16))
        totals = totals + partial_value.astype(jnp.float32)
    return totals

def channel_half(latent_representations, perceptron_switch_coefficients, perceptron_expand_coefficients, perceptron_contract_coefficients):
    gate_sum = jnp.dot(latent_representations, perceptron_switch_coefficients, preferred_element_type=jnp.float32)
    up_sum = jnp.dot(latent_representations, perceptron_expand_coefficients, preferred_element_type=jnp.float32)
    hidden = (jax.nn.silu(gate_sum) * up_sum).astype(jnp.bfloat16)
    return post_norm(latent_representations, 0.5 * rounded_sum(hidden, perceptron_contract_coefficients))

def linear_attention(queries, key_rows, values, forgetting_euler_power):
    token_count = queries.shape[0]
    seq_count = token_count // SEQUENCE_LENGTH

    def by_position(source, channels):
        shaped = source.astype(jnp.float32).reshape(seq_count, SEQUENCE_LENGTH, HEADS, channels)
        return shaped.transpose(1, 0, 2, 3)
    inputs = (by_position(queries, DK), by_position(key_rows, DK), by_position(values, DV), jnp.exp(by_position(forgetting_euler_power, DK)))
    start_state = jnp.zeros((seq_count, HEADS, DK, DV), jnp.float32)

    def forward(carried, step_in):
        query_now, key_now, value_now, decay_now = step_in
        carried = decay_now[..., None] * carried + key_now[..., None] * value_now[..., None, :]
        return (carried, jnp.einsum('shd,shdv->shv', query_now, carried, precision=highest))

    def reverse_direction_sweep(carried, step_in):
        query_now, key_now, value_now, decay_now = step_in
        seen = decay_now[..., None] * carried
        return (seen + key_now[..., None] * value_now[..., None, :], jnp.einsum('shd,shdv->shv', query_now, seen, precision=highest))
    _, from_before = lax.scan(forward, start_state, inputs)
    _, from_after = lax.scan(reverse_direction_sweep, start_state, inputs, reverse=True)
    return (from_before + from_after).transpose(1, 0, 2, 3).reshape(token_count, HEADS, DV)

def recurrent_context_blender(latent_representations, probe_coefficients, address_coefficients, payload_coefficients, emit_switch_coefficients, forgetting_shrink_coefficients, forgetting_expand_coefficients, forgetting_sigmoid_intercept, extra_forgetting_logits, subspace_rescaling_amplitude, recurrence_emit_coefficients):
    queries = jnp.dot(latent_representations, probe_coefficients, preferred_element_type=jnp.float32).astype(jnp.bfloat16)
    key_rows = jnp.dot(latent_representations, address_coefficients, preferred_element_type=jnp.float32).astype(jnp.bfloat16)
    values = jnp.dot(latent_representations, payload_coefficients, preferred_element_type=jnp.float32).astype(jnp.bfloat16)
    outgate = jnp.dot(latent_representations, emit_switch_coefficients, preferred_element_type=jnp.float32).astype(jnp.bfloat16)
    compact_inner_dimensionality = jnp.dot(latent_representations, forgetting_shrink_coefficients, preferred_element_type=jnp.float32).astype(jnp.bfloat16)
    forgetting_euler_power = jax.nn.log_sigmoid(jnp.dot(compact_inner_dimensionality, forgetting_expand_coefficients, preferred_element_type=jnp.float32) + forgetting_sigmoid_intercept) / forgetting_steepness_multiplier + extra_forgetting_logits
    mixed_heads = linear_attention(queries, key_rows, values, forgetting_euler_power)
    scaled = mixed_heads * lax.rsqrt(lax.optimization_barrier(jnp.mean(mixed_heads * mixed_heads, axis=-1, keepdims=True)) + epsilon) * subspace_rescaling_amplitude
    opener = jax.nn.silu(outgate.astype(jnp.float32)).reshape(mixed_heads.shape)
    gated = (scaled * opener).reshape(mixed_heads.shape[0], HEADS * DV).astype(jnp.bfloat16)
    return post_norm(latent_representations, rounded_sum(gated, recurrence_emit_coefficients))

def reference(incoming_representations, perceptron_switch_coefficients, perceptron_expand_coefficients, perceptron_contract_coefficients, probe_coefficients, address_coefficients, payload_coefficients, emit_switch_coefficients, forgetting_shrink_coefficients, forgetting_expand_coefficients, forgetting_sigmoid_intercept, extra_forgetting_logits, subspace_rescaling_amplitude, recurrence_emit_coefficients):
    opening_perceptron_result = channel_half(incoming_representations, perceptron_switch_coefficients, perceptron_expand_coefficients, perceptron_contract_coefficients)
    context_blend_result = recurrent_context_blender(opening_perceptron_result, probe_coefficients, address_coefficients, payload_coefficients, emit_switch_coefficients, forgetting_shrink_coefficients, forgetting_expand_coefficients, forgetting_sigmoid_intercept, extra_forgetting_logits, subspace_rescaling_amplitude, recurrence_emit_coefficients)
    return channel_half(context_blend_result, perceptron_switch_coefficients, perceptron_expand_coefficients, perceptron_contract_coefficients)
```

```python
import jax
import jax.numpy as jnp
from jax import lax
from jax.experimental import pallas as pl
from jax.experimental.pallas import tpu as pltpu
from jax.sharding import PartitionSpec as P

DK = 64
DV = 128
SUB = 16
SEQUENCE_LENGTH = 320
IN_FLIGHT = 3

residual_gain = 1.681792830507429
forgetting_steepness_multiplier = 16.0
epsilon = 1e-06
highest = lax.Precision.HIGHEST


def post_norm(residual, branch):
    summed = residual_gain * residual.astype(jnp.float32) + branch
    average = jnp.mean(summed, axis=-1, keepdims=True)
    centred = summed - average
    variance = jnp.mean(centred * centred, axis=-1, keepdims=True)
    return (centred * lax.rsqrt(variance + epsilon)).astype(jnp.bfloat16)


def mixing_kernel(q_ref, k_ref, v_ref, og_ref, ld_ref, gain_ref, out_ref, incl_ref, excl_ref, li_ref, le_ref):
    length, width = q_ref.shape
    heads = width // DK
    f32 = jnp.float32
    bf16 = jnp.bfloat16
    decay = ld_ref[...]
    row = lax.broadcasted_iota(jnp.int32, (length, length), 0)
    col = lax.broadcasted_iota(jnp.int32, (length, length), 1)
    row_blk = row // SUB
    col_blk = col // SUB
    within = jnp.where((row_blk == col_blk) & (col <= row), 1.0, 0.0).astype(f32)
    before = jnp.where(col_blk < row_blk, 1.0, 0.0).astype(f32)
    local = jnp.dot(within, decay, precision=highest, preferred_element_type=f32)
    offset = jnp.dot(before, decay, precision=highest, preferred_element_type=f32)
    li_ref[...] = local
    le_ref[...] = local - decay
    incl_ref[...] = offset + local
    excl_ref[...] = offset + (local - decay)
    lane_head = lax.broadcasted_iota(jnp.int32, (1, width), 1) // DK
    spread_row = lax.broadcasted_iota(jnp.int32, (width, heads * DV), 0) // DK
    spread_col = lax.broadcasted_iota(jnp.int32, (width, heads * DV), 1) // DV
    to_values = jnp.where(spread_row == spread_col, 1.0, 0.0).astype(bf16)
    key_pos = lax.broadcasted_iota(jnp.int32, (length, 1), 0)
    score_pos = lax.broadcasted_iota(jnp.int32, (heads * SUB, length), 1)
    shape3 = (SUB, SUB, width)
    lower = lax.broadcasted_iota(jnp.int32, shape3, 1) >= lax.broadcasted_iota(jnp.int32, shape3, 0)
    gain = gain_ref[...]

    def block(i, carry):
        start = pl.multiple_of(i * SUB, SUB)
        rows = pl.ds(start, SUB)
        q = q_ref[rows, :].astype(f32)
        k = k_ref[rows, :].astype(f32)
        v = v_ref[rows, :].astype(f32)
        li = li_ref[rows, :]
        le = le_ref[rows, :]
        total = li[SUB - 1 :, :]
        first = excl_ref[rows, :][:1, :]
        last = first + total
        earlier = key_pos < start
        inside = (key_pos >= start) & (key_pos < start + SUB)
        power = jnp.where(earlier, first - incl_ref[...], excl_ref[...] - last)
        scale = jnp.where(inside, 0.0, jnp.exp(jnp.minimum(power, 0.0)))
        keys = (k_ref[...].astype(f32) * scale).astype(bf16)
        q_fwd = q * jnp.exp(li)
        q_bwd = q * jnp.exp(total - le)
        stack = [jnp.where(lane_head == h, q_fwd, 0.0) for h in range(heads)]
        stack += [jnp.where(lane_head == h, q_bwd, 0.0) for h in range(heads)]
        probe = jnp.concatenate(stack, axis=0).astype(bf16)
        both = lax.dot_general(probe, keys, (((1,), (1,)), ((), ())), preferred_element_type=f32)
        score = jnp.where(score_pos < start, both[: heads * SUB], both[heads * SUB :]).astype(bf16)
        far = jnp.dot(score, v_ref[...], preferred_element_type=f32)
        far = jnp.concatenate(
            [far[h * SUB : (h + 1) * SUB, h * DV : (h + 1) * DV] for h in range(heads)], axis=1
        )
        gap = jnp.where(lower, li[None, :, :] - li[:, None, :], le[:, None, :] - le[None, :, :])
        near = (q[None, :, :] * k[:, None, :] * jnp.exp(gap)).astype(bf16)
        weight = jnp.dot(near.reshape(SUB * SUB, width), to_values, preferred_element_type=f32)
        weight = weight.reshape(SUB, SUB, heads * DV)
        mixed = far + jnp.sum(weight * v[:, None, :], axis=0)
        og = og_ref[rows, :].astype(f32)
        opener = og / (1.0 + jnp.exp(-og))
        pieces = []
        for h in range(heads):
            part = mixed[:, h * DV : (h + 1) * DV]
            power_mean = jnp.mean(part * part, axis=-1, keepdims=True)
            pieces.append(part * lax.rsqrt(power_mean + epsilon) * gain)
        out_ref[rows, :] = (jnp.concatenate(pieces, axis=1) * opener).astype(bf16)
        return carry

    lax.fori_loop(0, length // SUB, block, 0, unroll=2)


def mix(queries, key_rows, values, outgate, log_decay, gain):
    tokens, width = queries.shape
    wide = values.shape[1]
    seq = SEQUENCE_LENGTH
    narrow_spec = pl.BlockSpec((seq, width), lambda s: (s, 0))
    wide_spec = pl.BlockSpec((seq, wide), lambda s: (s, 0))
    return pl.pallas_call(
        mixing_kernel,
        grid=(tokens // seq,),
        in_specs=[
            narrow_spec,
            narrow_spec,
            wide_spec,
            wide_spec,
            narrow_spec,
            pl.BlockSpec((1, DV), lambda s: (0, 0)),
        ],
        out_specs=wide_spec,
        out_shape=jax.ShapeDtypeStruct((tokens, wide), jnp.bfloat16),
        scratch_shapes=[pltpu.VMEM((seq, width), jnp.float32) for _ in range(4)],
        cost_estimate=pl.CostEstimate(
            flops=tokens * 400000, transcendentals=tokens * 4000, bytes_accessed=tokens * width * 16
        ),
        name="mixing",
    )(queries, key_rows, values, outgate, log_decay, gain.reshape(1, DV))


def make_per_device(mesh):
    n_fs = mesh.shape["fs"]
    n_tp = mesh.shape["tp"]
    n_grp = mesh.shape["grp"]
    cores = 2 if n_tp % 2 == 0 else 1
    n_x = n_tp // cores

    def shift(value, axis, step):
        size = mesh.shape[axis]
        return lax.ppermute(value, axis, [((i + step) % size, i) for i in range(size)])

    def from_x(value, step):
        hop = step * cores
        return lax.ppermute(value, "tp", [((i + hop) % n_tp, i) for i in range(n_tp)])

    def from_core(value):
        return lax.ppermute(value, "tp", [(i ^ 1, i) for i in range(n_tp)])

    def per_device(x, w_gate, w_up, w_down, w_q, w_k, w_v, w_g, w_shrink, w_expand, intercept, extra, gain, w_out):
        fs = lax.axis_index("fs")
        grp = lax.axis_index("grp")
        core = lax.axis_index("tp") % cores
        x_pos = lax.axis_index("tp") // cores

        def reorder(value, axis, inverse=False):
            size = value.shape[axis]
            stripe = size // n_fs
            part = stripe // n_grp

            def roll_stripes(v, amount):
                doubled = jnp.concatenate([v, v], axis=axis)
                return lax.dynamic_slice_in_dim(doubled, amount * stripe, size, axis=axis)

            def roll_parts(v, amount):
                result = v
                for a in range(1, n_grp):
                    rolled = jnp.concatenate(
                        [
                            lax.slice_in_dim(
                                v,
                                s * stripe + ((p + a) % n_grp) * part,
                                s * stripe + ((p + a) % n_grp + 1) * part,
                                axis=axis,
                            )
                            for s in range(n_fs)
                            for p in range(n_grp)
                        ],
                        axis=axis,
                    )
                    result = jnp.where(amount == a, rolled, result)
                return result

            if inverse:
                return roll_stripes(roll_parts(value, (n_grp - grp) % n_grp), (n_fs - fs) % n_fs)
            return roll_parts(roll_stripes(value, fs), grp)

        history = []

        def paced(value, step):
            if len(history) >= IN_FLIGHT:
                value, _ = lax.optimization_barrier((value, history[-IN_FLIGHT]))
            result = shift(value, "fs", step)
            history.append(result)
            return result

        def gather_many(weights, axes):
            parts = []
            for w, axis in zip(weights, axes):
                part = w.shape[axis] // n_grp
                parts.append(
                    [
                        lax.dynamic_slice_in_dim(w, ((grp + j) % n_grp) * part, part, axis=axis)
                        for j in range(n_grp)
                    ]
                )
            own = [{0: p[0]} for p in parts]
            ahead = n_fs // 2
            for k in range(1, ahead + 1):
                for o in own:
                    o[k] = paced(o[k - 1], 1)
                back = n_fs - k
                if back > ahead:
                    for o in own:
                        o[back] = paced(o[(back + 1) % n_fs], -1)
            stripes = []
            for w_index, axis in enumerate(axes):
                one = []
                for k in range(n_fs):
                    if k == 0:
                        pieces = parts[w_index]
                    else:
                        mine = own[w_index][k]
                        pieces = [mine] + [shift(mine, "grp", j) for j in range(1, n_grp)]
                    one.append(pieces)
                stripes.append(one)
            return stripes

        def assemble(one, axis):
            return jnp.concatenate([p for pieces in one for p in pieces], axis=axis)

        def gather_rows(stored):
            chunks = []
            for s in range(n_x):
                mine = stored if s == 0 else from_x(stored, s)
                chunks.append(jnp.concatenate([mine, from_core(mine)], axis=0) if cores == 2 else mine)
            return chunks

        def core_major(chunks, rows):
            if len(chunks) == 1:
                return chunks[0]
            return jnp.concatenate(
                [c[d * rows : (d + 1) * rows] for d in range(cores) for c in chunks], axis=0
            )

        def return_rows(hidden, stripes, rows):
            outs = []
            for piece in stripes:
                partial = jnp.dot(hidden, piece, preferred_element_type=jnp.float32).astype(jnp.bfloat16)
                total = partial[: n_x * rows].astype(jnp.float32)
                if cores == 2:
                    total = total + from_core(partial[n_x * rows :]).astype(jnp.float32)
                narrow = total.astype(jnp.bfloat16)
                result = total[:rows]
                for s in range(1, n_x):
                    result = result + from_x(narrow[s * rows : (s + 1) * rows], -s).astype(jnp.float32)
                outs.append(result)
            return jnp.concatenate(outs, axis=1)

        rows = x.shape[0]
        x_own = reorder(x, 1)
        x_chunks = gather_rows(x_own)
        gate_p, up_p = gather_many([w_gate, w_up], [0, 0])
        (down_p,) = gather_many([w_down], [1])
        w_qkvg = jnp.concatenate([w_q, w_k, w_v, w_g], axis=1)
        (qkvg_p,) = gather_many([w_qkvg], [0])
        (out_p,) = gather_many([w_out], [1])
        gate_full = assemble(gate_p, 0)
        up_full = assemble(up_p, 0)
        down_full = [jnp.concatenate(p, axis=1) for p in down_p]
        qkvg_full = assemble(qkvg_p, 0)
        out_full = [jnp.concatenate(p, axis=1) for p in out_p]
        shrink = reorder(w_shrink, 0)

        def hidden_of(chunk):
            gate_sum = jnp.dot(chunk, gate_full, preferred_element_type=jnp.float32)
            up_sum = jnp.dot(chunk, up_full, preferred_element_type=jnp.float32)
            return (jax.nn.silu(gate_sum) * up_sum).astype(jnp.bfloat16)

        hidden = hidden_of(core_major(x_chunks, rows))
        first = post_norm(x_own, 0.5 * return_rows(hidden, down_full, rows))

        dk_wide = w_q.shape[1]
        dv_wide = w_v.shape[1]

        def to_order(chunks):
            done = []
            for c in chunks:
                if cores == 2:
                    swapped = jnp.concatenate([c[rows:], c[:rows]], axis=0)
                    c = jnp.where(core == 0, c, swapped)
                done.append(c)
            joined = jnp.concatenate(done, axis=0) if len(done) > 1 else done[0]
            if (cores * rows) % SEQUENCE_LENGTH == 0:
                return joined
            doubled = jnp.concatenate([joined, joined], axis=0)
            return lax.dynamic_slice_in_dim(
                doubled, ((n_x - x_pos) % n_x) * cores * rows, joined.shape[0], axis=0
            )

        def from_order(joined):
            if (cores * rows) % SEQUENCE_LENGTH != 0:
                doubled = jnp.concatenate([joined, joined], axis=0)
                joined = lax.dynamic_slice_in_dim(
                    doubled, x_pos * cores * rows, joined.shape[0], axis=0
                )
            chunks = []
            for s in range(n_x):
                c = joined[s * cores * rows : (s + 1) * cores * rows]
                if cores == 2:
                    swapped = jnp.concatenate([c[rows:], c[:rows]], axis=0)
                    c = jnp.where(core == 0, c, swapped)
                chunks.append(c)
            return core_major(chunks, rows)

        extra_order = extra
        if (cores * rows) % SEQUENCE_LENGTH == 0:
            doubled = jnp.concatenate([extra, extra], axis=0)
            extra_order = lax.dynamic_slice_in_dim(
                doubled, x_pos * cores * rows, extra.shape[0], axis=0
            )

        projected = []
        compact = []
        for chunk in gather_rows(first):
            projected.append(
                jnp.dot(chunk, qkvg_full, preferred_element_type=jnp.float32).astype(jnp.bfloat16)
            )
            compact.append(
                jnp.dot(chunk, shrink, preferred_element_type=jnp.float32).astype(jnp.bfloat16)
            )
        projected = to_order(projected)
        compact = to_order(compact)
        log_decay = (
            jax.nn.log_sigmoid(
                jnp.dot(compact, w_expand, preferred_element_type=jnp.float32) + intercept
            )
            / forgetting_steepness_multiplier
            + extra_order
        )
        gated = mix(
            projected[:, :dk_wide],
            projected[:, dk_wide : 2 * dk_wide],
            projected[:, 2 * dk_wide : 2 * dk_wide + dv_wide],
            projected[:, 2 * dk_wide + dv_wide :],
            log_decay,
            gain,
        )
        second = post_norm(first, return_rows(from_order(gated), out_full, rows))
        hidden = core_major([hidden_of(c) for c in gather_rows(second)], rows)
        third = post_norm(second, 0.5 * return_rows(hidden, down_full, rows))
        return reorder(third, 1, inverse=True)

    return per_device


def solution(mesh):
    return jax.shard_map(
        make_per_device(mesh),
        mesh=mesh,
        in_specs=(
            P(("grp", "fs", "tp"), None),
            P("fs", "tp"),
            P("fs", "tp"),
            P("tp", "fs"),
            P("fs", "tp"),
            P("fs", "tp"),
            P("fs", "tp"),
            P("fs", "tp"),
            P(),
            P(None, "tp"),
            P("tp"),
            P(("grp", "fs"), "tp"),
            P(),
            P("tp", "fs"),
        ),
        out_specs=P(("grp", "fs", "tp"), None),
        check_vma=False,
    )
```

```python
import jax
import jax.numpy as jnp
from jax import lax
from jax.experimental import pallas as pl
from jax.experimental.pallas import tpu as pltpu
from jax.sharding import PartitionSpec as P

DK = 64
DV = 128
SUB = 16
SEQUENCE_LENGTH = 320
IN_FLIGHT = 2

residual_gain = 1.681792830507429
forgetting_steepness_multiplier = 16.0
epsilon = 1e-06
highest = lax.Precision.HIGHEST


def post_norm(residual, branch):
    summed = residual_gain * residual.astype(jnp.float32) + branch
    average = jnp.mean(summed, axis=-1, keepdims=True)
    centred = summed - average
    variance = jnp.mean(centred * centred, axis=-1, keepdims=True)
    return (centred * lax.rsqrt(variance + epsilon)).astype(jnp.bfloat16)


def mixing_kernel(q_ref, k_ref, v_ref, og_ref, ld_ref, gain_ref, out_ref, incl_ref, excl_ref, li_ref, le_ref):
    length, width = q_ref.shape
    heads = width // DK
    f32 = jnp.float32
    bf16 = jnp.bfloat16
    decay = ld_ref[...]
    row = lax.broadcasted_iota(jnp.int32, (length, length), 0)
    col = lax.broadcasted_iota(jnp.int32, (length, length), 1)
    row_blk = row // SUB
    col_blk = col // SUB
    within = jnp.where((row_blk == col_blk) & (col <= row), 1.0, 0.0).astype(f32)
    before = jnp.where(col_blk < row_blk, 1.0, 0.0).astype(f32)
    local = jnp.dot(within, decay, precision=highest, preferred_element_type=f32)
    offset = jnp.dot(before, decay, precision=highest, preferred_element_type=f32)
    li_ref[...] = local
    le_ref[...] = local - decay
    incl_ref[...] = offset + local
    excl_ref[...] = offset + (local - decay)
    lane_head = lax.broadcasted_iota(jnp.int32, (1, width), 1) // DK
    spread_row = lax.broadcasted_iota(jnp.int32, (width, heads * DV), 0) // DK
    spread_col = lax.broadcasted_iota(jnp.int32, (width, heads * DV), 1) // DV
    to_values = jnp.where(spread_row == spread_col, 1.0, 0.0).astype(bf16)
    key_pos = lax.broadcasted_iota(jnp.int32, (length, 1), 0)
    score_pos = lax.broadcasted_iota(jnp.int32, (heads * SUB, length), 1)
    shape3 = (SUB, SUB, width)
    lower = lax.broadcasted_iota(jnp.int32, shape3, 1) >= lax.broadcasted_iota(jnp.int32, shape3, 0)
    gain = gain_ref[...]

    def block(i, carry):
        start = pl.multiple_of(i * SUB, SUB)
        rows = pl.ds(start, SUB)
        q = q_ref[rows, :].astype(f32)
        k = k_ref[rows, :].astype(f32)
        v = v_ref[rows, :].astype(f32)
        li = li_ref[rows, :]
        le = le_ref[rows, :]
        total = li[SUB - 1 :, :]
        first = excl_ref[rows, :][:1, :]
        last = first + total
        earlier = key_pos < start
        inside = (key_pos >= start) & (key_pos < start + SUB)
        power = jnp.where(earlier, first - incl_ref[...], excl_ref[...] - last)
        scale = jnp.where(inside, 0.0, jnp.exp(jnp.minimum(power, 0.0)))
        keys = (k_ref[...].astype(f32) * scale).astype(bf16)
        q_fwd = q * jnp.exp(li)
        q_bwd = q * jnp.exp(total - le)
        stack = [jnp.where(lane_head == h, q_fwd, 0.0) for h in range(heads)]
        stack += [jnp.where(lane_head == h, q_bwd, 0.0) for h in range(heads)]
        probe = jnp.concatenate(stack, axis=0).astype(bf16)
        both = lax.dot_general(probe, keys, (((1,), (1,)), ((), ())), preferred_element_type=f32)
        score = jnp.where(score_pos < start, both[: heads * SUB], both[heads * SUB :]).astype(bf16)
        far = jnp.dot(score, v_ref[...], preferred_element_type=f32)
        far = jnp.concatenate(
            [far[h * SUB : (h + 1) * SUB, h * DV : (h + 1) * DV] for h in range(heads)], axis=1
        )
        gap = jnp.where(lower, li[None, :, :] - li[:, None, :], le[:, None, :] - le[None, :, :])
        near = (q[None, :, :] * k[:, None, :] * jnp.exp(gap)).astype(bf16)
        weight = jnp.dot(near.reshape(SUB * SUB, width), to_values, preferred_element_type=f32)
        weight = weight.reshape(SUB, SUB, heads * DV)
        mixed = far + jnp.sum(weight * v[:, None, :], axis=0)
        og = og_ref[rows, :].astype(f32)
        opener = og / (1.0 + jnp.exp(-og))
        pieces = []
        for h in range(heads):
            part = mixed[:, h * DV : (h + 1) * DV]
            power_mean = jnp.mean(part * part, axis=-1, keepdims=True)
            pieces.append(part * lax.rsqrt(power_mean + epsilon) * gain)
        out_ref[rows, :] = (jnp.concatenate(pieces, axis=1) * opener).astype(bf16)
        return carry

    lax.fori_loop(0, length // SUB, block, 0, unroll=2)


def mix(queries, key_rows, values, outgate, log_decay, gain):
    tokens, width = queries.shape
    wide = values.shape[1]
    seq = SEQUENCE_LENGTH
    narrow_spec = pl.BlockSpec((seq, width), lambda s: (s, 0))
    wide_spec = pl.BlockSpec((seq, wide), lambda s: (s, 0))
    return pl.pallas_call(
        mixing_kernel,
        grid=(tokens // seq,),
        in_specs=[
            narrow_spec,
            narrow_spec,
            wide_spec,
            wide_spec,
            narrow_spec,
            pl.BlockSpec((1, DV), lambda s: (0, 0)),
        ],
        out_specs=wide_spec,
        out_shape=jax.ShapeDtypeStruct((tokens, wide), jnp.bfloat16),
        scratch_shapes=[pltpu.VMEM((seq, width), jnp.float32) for _ in range(4)],
        cost_estimate=pl.CostEstimate(
            flops=tokens * 400000, transcendentals=tokens * 4000, bytes_accessed=tokens * width * 16
        ),
        name="mixing",
    )(queries, key_rows, values, outgate, log_decay, gain.reshape(1, DV))


def make_per_device(mesh):
    n_fs = mesh.shape["fs"]
    n_tp = mesh.shape["tp"]
    n_grp = mesh.shape["grp"]
    cores = 2 if n_tp % 2 == 0 else 1
    n_x = n_tp // cores

    def shift(value, axis, step):
        size = mesh.shape[axis]
        return lax.ppermute(value, axis, [((i + step) % size, i) for i in range(size)])

    def from_x(value, step):
        hop = step * cores
        return lax.ppermute(value, "tp", [((i + hop) % n_tp, i) for i in range(n_tp)])

    def from_core(value):
        return lax.ppermute(value, "tp", [(i ^ 1, i) for i in range(n_tp)])

    def per_device(x, w_gate, w_up, w_down, w_q, w_k, w_v, w_g, w_shrink, w_expand, intercept, extra, gain, w_out):
        fs = lax.axis_index("fs")
        grp = lax.axis_index("grp")
        core = lax.axis_index("tp") % cores
        x_pos = lax.axis_index("tp") // cores

        def reorder(value, axis, inverse=False):
            size = value.shape[axis]
            stripe = size // n_fs
            part = stripe // n_grp

            def roll_stripes(v, amount):
                doubled = jnp.concatenate([v, v], axis=axis)
                return lax.dynamic_slice_in_dim(doubled, amount * stripe, size, axis=axis)

            def roll_parts(v, amount):
                result = v
                for a in range(1, n_grp):
                    rolled = jnp.concatenate(
                        [
                            lax.slice_in_dim(
                                v,
                                s * stripe + ((p + a) % n_grp) * part,
                                s * stripe + ((p + a) % n_grp + 1) * part,
                                axis=axis,
                            )
                            for s in range(n_fs)
                            for p in range(n_grp)
                        ],
                        axis=axis,
                    )
                    result = jnp.where(amount == a, rolled, result)
                return result

            if inverse:
                return roll_stripes(roll_parts(value, (n_grp - grp) % n_grp), (n_fs - fs) % n_fs)
            return roll_parts(roll_stripes(value, fs), grp)

        history = []

        def paced(value, step):
            if len(history) >= IN_FLIGHT:
                value, _ = lax.optimization_barrier((value, history[-IN_FLIGHT]))
            result = shift(value, "fs", step)
            history.append(result)
            return result

        def gather_many(weights, axes):
            parts = []
            for w, axis in zip(weights, axes):
                part = w.shape[axis] // n_grp
                parts.append(
                    [
                        lax.dynamic_slice_in_dim(w, ((grp + j) % n_grp) * part, part, axis=axis)
                        for j in range(n_grp)
                    ]
                )
            own = [{0: p[0]} for p in parts]
            ahead = n_fs // 2
            for k in range(1, ahead + 1):
                for o in own:
                    o[k] = paced(o[k - 1], 1)
                back = n_fs - k
                if back > ahead:
                    for o in own:
                        o[back] = paced(o[(back + 1) % n_fs], -1)
            stripes = []
            for w_index, axis in enumerate(axes):
                one = []
                for k in range(n_fs):
                    if k == 0:
                        pieces = parts[w_index]
                    else:
                        mine = own[w_index][k]
                        pieces = [mine] + [shift(mine, "grp", j) for j in range(1, n_grp)]
                    one.append(pieces)
                stripes.append(one)
            return stripes

        def assemble(one, axis):
            return jnp.concatenate([p for pieces in one for p in pieces], axis=axis)

        def gather_rows(stored):
            chunks = []
            for s in range(n_x):
                mine = stored if s == 0 else from_x(stored, s)
                chunks.append(jnp.concatenate([mine, from_core(mine)], axis=0) if cores == 2 else mine)
            return chunks

        def core_major(chunks, rows):
            if len(chunks) == 1:
                return chunks[0]
            return jnp.concatenate(
                [c[d * rows : (d + 1) * rows] for d in range(cores) for c in chunks], axis=0
            )

        def return_rows(hidden, stripes, rows):
            outs = []
            for piece in stripes:
                partial = jnp.dot(hidden, piece, preferred_element_type=jnp.float32).astype(jnp.bfloat16)
                total = partial[: n_x * rows].astype(jnp.float32)
                if cores == 2:
                    total = total + from_core(partial[n_x * rows :]).astype(jnp.float32)
                narrow = total.astype(jnp.bfloat16)
                result = total[:rows]
                for s in range(1, n_x):
                    result = result + from_x(narrow[s * rows : (s + 1) * rows], -s).astype(jnp.float32)
                outs.append(result)
            return jnp.concatenate(outs, axis=1)

        rows = x.shape[0]
        x_own = reorder(x, 1)
        x_chunks = gather_rows(x_own)
        (gate_p,) = gather_many([w_gate], [0])
        (up_p,) = gather_many([w_up], [0])
        (down_p,) = gather_many([w_down], [1])
        w_qkvg = jnp.concatenate([w_q, w_k, w_v, w_g], axis=1)
        (qkvg_p,) = gather_many([w_qkvg], [0])
        (out_p,) = gather_many([w_out], [1])
        gate_full = assemble(gate_p, 0)
        up_full = assemble(up_p, 0)
        down_full = [jnp.concatenate(p, axis=1) for p in down_p]
        qkvg_full = assemble(qkvg_p, 0)
        out_full = [jnp.concatenate(p, axis=1) for p in out_p]
        shrink = reorder(w_shrink, 0)

        def hidden_of(chunk):
            gate_sum = jnp.dot(chunk, gate_full, preferred_element_type=jnp.float32)
            up_sum = jnp.dot(chunk, up_full, preferred_element_type=jnp.float32)
            return (jax.nn.silu(gate_sum) * up_sum).astype(jnp.bfloat16)

        hidden = hidden_of(core_major(x_chunks, rows))
        first = post_norm(x_own, 0.5 * return_rows(hidden, down_full, rows))

        dk_wide = w_q.shape[1]
        dv_wide = w_v.shape[1]

        def to_order(chunks):
            done = []
            for c in chunks:
                if cores == 2:
                    swapped = jnp.concatenate([c[rows:], c[:rows]], axis=0)
                    c = jnp.where(core == 0, c, swapped)
                done.append(c)
            joined = jnp.concatenate(done, axis=0) if len(done) > 1 else done[0]
            if (cores * rows) % SEQUENCE_LENGTH == 0:
                return joined
            doubled = jnp.concatenate([joined, joined], axis=0)
            return lax.dynamic_slice_in_dim(
                doubled, ((n_x - x_pos) % n_x) * cores * rows, joined.shape[0], axis=0
            )

        def from_order(joined):
            if (cores * rows) % SEQUENCE_LENGTH != 0:
                doubled = jnp.concatenate([joined, joined], axis=0)
                joined = lax.dynamic_slice_in_dim(
                    doubled, x_pos * cores * rows, joined.shape[0], axis=0
                )
            chunks = []
            for s in range(n_x):
                c = joined[s * cores * rows : (s + 1) * cores * rows]
                if cores == 2:
                    swapped = jnp.concatenate([c[rows:], c[:rows]], axis=0)
                    c = jnp.where(core == 0, c, swapped)
                chunks.append(c)
            return core_major(chunks, rows)

        extra_order = extra
        if (cores * rows) % SEQUENCE_LENGTH == 0:
            doubled = jnp.concatenate([extra, extra], axis=0)
            extra_order = lax.dynamic_slice_in_dim(
                doubled, x_pos * cores * rows, extra.shape[0], axis=0
            )

        projected = []
        compact = []
        for chunk in gather_rows(first):
            projected.append(
                jnp.dot(chunk, qkvg_full, preferred_element_type=jnp.float32).astype(jnp.bfloat16)
            )
            compact.append(
                jnp.dot(chunk, shrink, preferred_element_type=jnp.float32).astype(jnp.bfloat16)
            )
        projected = to_order(projected)
        compact = to_order(compact)
        log_decay = (
            jax.nn.log_sigmoid(
                jnp.dot(compact, w_expand, preferred_element_type=jnp.float32) + intercept
            )
            / forgetting_steepness_multiplier
            + extra_order
        )
        gated = mix(
            projected[:, :dk_wide],
            projected[:, dk_wide : 2 * dk_wide],
            projected[:, 2 * dk_wide : 2 * dk_wide + dv_wide],
            projected[:, 2 * dk_wide + dv_wide :],
            log_decay,
            gain,
        )
        second = post_norm(first, return_rows(from_order(gated), out_full, rows))
        hidden = core_major([hidden_of(c) for c in gather_rows(second)], rows)
        third = post_norm(second, 0.5 * return_rows(hidden, down_full, rows))
        return reorder(third, 1, inverse=True)

    return per_device


def solution(mesh):
    return jax.shard_map(
        make_per_device(mesh),
        mesh=mesh,
        in_specs=(
            P(("grp", "fs", "tp"), None),
            P("fs", "tp"),
            P("fs", "tp"),
            P("tp", "fs"),
            P("fs", "tp"),
            P("fs", "tp"),
            P("fs", "tp"),
            P("fs", "tp"),
            P(),
            P(None, "tp"),
            P("tp"),
            P(("grp", "fs"), "tp"),
            P(),
            P("tp", "fs"),
        ),
        out_specs=P(("grp", "fs", "tp"), None),
        check_vma=False,
    )
```
